32 devices in a mesh: sp: 16 (over z, y, x), tp: 2 (over core).
Axes of the slice: x: 2, y: 2, z: 4, core: 2. Of those that a mesh axis runs over, the one named last changes fastest.
Arguments:
- value_in: bfloat16 [5760, 2048], P('sp', 'tp'), may hold values from -240 to 240
- gate_in: bfloat16 [5760, 2048], P('sp', 'tp'), may hold values from -8 to 8
- taps: float32 [31, 2048], P(None, 'tp'), may hold values from -1 to 1
- norm_gain: float32 [2048], P('tp'), may hold values from 0.1 to 1.9
- norm_bias: float32 [2048], P('tp'), may hold values from -3 to 3
- proj_weight: bfloat16 [2048, 4096], P('tp', 'sp'), may hold values from -0.125 to 0.125
- out_grad: bfloat16 [5760, 4096], P('sp'), may hold values from -6 to 6
Outputs:
- value_grad: bfloat16 [5760, 2048], P('sp', 'tp')
- gate_grad: bfloat16 [5760, 2048], P('sp', 'tp')
- tap_grad: float32 [31, 2048], P(None, 'tp')
- gain_grad: float32 [2048], P('tp')
- bias_grad: float32 [2048], P('tp')
- weight_grad: float32 [2048, 4096], P('tp', 'sp')
The draws below stay inside these ranges and needn't reach their ends.
All inputs are finite; a program needn't handle non-finite values.
Results may differ from the reference program's by a relative error of at most 0.0051.
Values may be sent and summed in bfloat16 or wider, within the bound.
No kernel may reach another device: no remote copies, remote signals or barrier semaphores. Data moves between devices by JAX's collectives and lax.ppermute only.
A program may use at most 64 MiB of HBM per device.

```python
import math
import jax
import jax.numpy as jnp
from jax import lax

MODEL = 4096
CHANNELS = 2048
TAPS = 31
TOKENS = 5760


def draw_value_in(key, part):
    first, second = jax.random.split(key, 2)
    chan = jnp.exp(jnp.linspace(0.0, math.log(10.0), CHANNELS)) * jax.random.uniform(second, (CHANNELS,), jnp.float32, 0.5, 2.0)
    along = jnp.exp(jnp.linspace(0.0, math.log(3.0), TOKENS))[:, None]
    base = jnp.clip(jax.random.normal(first, (TOKENS, CHANNELS), jnp.float32), -4.0, 4.0)
    return jnp.clip(base * chan[None, :] * along, -240.0, 240.0).astype(jnp.bfloat16)


def with_spikes(drawn, rng, source, target, blocks, factor):
    def block_of(position):
        return (jnp.arange(drawn.shape[position]) // (drawn.shape[position] // blocks)).reshape((-1,) + (1,) * (drawn.ndim - 1 - position))

    one_side = jax.random.permutation(rng, blocks)[block_of(target)]
    second = (block_of(target) + blocks // 2) % blocks
    return jnp.where((block_of(source) == one_side) | (block_of(source) == second), factor * drawn, drawn)


def levels(rng, shape, cuts, smallest, largest):
    loudness = 1.0
    for axis_at, shards_of in cuts:
        heights = jax.random.uniform(jax.random.fold_in(jax.random.fold_in(rng, 6), axis_at), (shards_of,), jnp.float32, smallest / len(cuts), largest / len(cuts))
        loudness = loudness * jnp.repeat(jnp.exp(heights), shape[axis_at] // shards_of).reshape((-1,) + (1,) * (len(shape) - 1 - axis_at))
    return loudness


def gaussian(key, dims, width, most, cuts=(), dtype=jnp.bfloat16):
    loudness = levels(key, dims, cuts, -0.22, 0.18) if cuts else 1.0
    values = jax.random.normal(key, dims, jnp.float32) * width * loudness
    return jnp.minimum(jnp.maximum(values, -most), most).astype(dtype)


def heavy_noise(stream_key, shape, scale, reach, cuts, heavy, kind=jnp.bfloat16):
    values = scale * jax.random.normal(stream_key, shape, jnp.float32)
    if cuts:
        values = values * levels(stream_key, shape, cuts, -0.22, 0.18)
    return jnp.clip(with_spikes(values, jax.random.fold_in(stream_key, 3), *heavy), -reach, reach).astype(kind)


def setup_inputs(seed: int = 0) -> dict:
    streams_of = jax.random.split(jax.random.key(seed), 8)
    return {
        "value_in": draw_value_in(jax.random.fold_in(streams_of[7], 71), 0),
        "gate_in": gaussian(streams_of[1], (TOKENS, CHANNELS), 2.0, 8.0, ((0, 16), (1, 2))),
        "taps": gaussian(streams_of[2], (TAPS, CHANNELS), TAPS ** -0.5, 1.0, ((1, 2),), jnp.float32),
        "norm_gain": jnp.clip(1.0 + 0.18 * jax.random.normal(streams_of[3], (CHANNELS,), jnp.float32), 0.1, 1.9),
        "norm_bias": gaussian(streams_of[4], (CHANNELS,), 0.5, 3.0, ((0, 2),), jnp.float32),
        "proj_weight": gaussian(streams_of[5], (CHANNELS, MODEL), CHANNELS ** -0.5, 0.125, ((0, 2), (1, 16))),
        "out_grad": heavy_noise(streams_of[6], (TOKENS, MODEL), 1.0, 6.0, ((0, 16),), (0, 1, 16, 2.0)),
    }


def reference(value_in, gate_in, taps, norm_gain, norm_bias, proj_weight, out_grad):
    f32 = jnp.float32
    rows = value_in.shape[0]
    span = taps.shape[0]
    half = span // 2
    width_all = value_in.shape[1]
    gate_sig = jax.nn.sigmoid(gate_in.astype(f32))
    value_f = value_in.astype(f32)
    mixed = (value_f * gate_sig).astype(jnp.bfloat16)
    padded = jnp.pad(mixed.astype(f32), ((half, half), (0, 0)))
    conv = jnp.zeros((rows, width_all), f32)
    for k in range(span):
        conv = conv + taps[k] * padded[k:k + rows]
    mean = lax.optimization_barrier(jnp.sum(conv, axis=1)) / width_all
    centred = conv - mean[:, None]
    spread = lax.optimization_barrier(jnp.sum(centred * centred, axis=1)) / width_all
    inv = lax.rsqrt(spread + 1e-06)
    normed = centred * inv[:, None]
    pre = normed * norm_gain + norm_bias
    act = jax.nn.silu(pre).astype(jnp.bfloat16)
    act_grad = lax.dot_general(out_grad, proj_weight, (((1,), (1,)), ((), ())), preferred_element_type=f32)
    weight_grad = lax.dot_general(act, out_grad, (((0,), (0,)), ((), ())), preferred_element_type=f32)
    sig_pre = jax.nn.sigmoid(pre)
    pre_grad = act_grad * sig_pre * (1.0 + pre * (1.0 - sig_pre))
    gain_grad = lax.optimization_barrier(jnp.sum(pre_grad * normed, axis=0))
    bias_grad = lax.optimization_barrier(jnp.sum(pre_grad, axis=0))
    normed_grad = pre_grad * norm_gain
    first = lax.optimization_barrier(jnp.sum(normed_grad, axis=1)) / width_all
    second = lax.optimization_barrier(jnp.sum(normed_grad * normed, axis=1)) / width_all
    conv_grad = inv[:, None] * (normed_grad - first[:, None] - normed * second[:, None])
    tap_grad = jnp.stack([lax.optimization_barrier(jnp.sum(conv_grad * padded[k:k + rows], axis=0)) for k in range(span)])
    grad_pad = jnp.pad(conv_grad, ((half, half), (0, 0)))
    mixed_grad = jnp.zeros((rows, width_all), f32)
    for k in range(span):
        mixed_grad = mixed_grad + taps[k] * grad_pad[2 * half - k:2 * half - k + rows]
    value_grad = (mixed_grad * gate_sig).astype(jnp.bfloat16)
    gate_grad = (mixed_grad * value_f * gate_sig * (1.0 - gate_sig)).astype(jnp.bfloat16)
    return (value_grad, gate_grad, tap_grad, gain_grad, bias_grad, weight_grad)
```

```python
import jax
import jax.numpy as jnp
from jax import lax
from jax.sharding import Mesh, PartitionSpec as P


SP = ("far", "near")


def padded_2(cells, axis, width):
    count = lax.axis_size(axis)
    ends = count - 1
    head = lax.slice_in_dim(cells, 0, width, axis=0)
    tail = lax.slice_in_dim(cells, cells.shape[0] - width, cells.shape[0], axis=0)
    return jnp.concatenate(
        [
            lax.ppermute(tail, axis, [(i, (i + 1) % count) for i in range(ends)]),
            cells,
            lax.ppermute(head, axis, [((i + 1) % count, i) for i in range(ends)]),
        ],
        axis=0,
    )


def exchange(blocks, axis):
    return lax.all_to_all(blocks, axis, split_axis=0, concat_axis=0)


def spread_out(block, axis):
    count = lax.axis_size(axis)
    return exchange(jnp.broadcast_to(block[None], (count,) + block.shape), axis)


def sum_over(parts, axis):
    count = lax.axis_size(axis)
    rows, width = parts.shape
    each = -(-rows // count)
    blocks = jnp.pad(parts, ((0, each * count - rows), (0, 0))).reshape(count, each, width)
    mine = jnp.sum(exchange(blocks, axis), axis=0)
    return spread_out(mine, axis).reshape(each * count, width)[:rows]


def paired(count):
    return count & (count - 1) == 0


def partner(index, step, count):
    return index ^ step if paired(count) else (index + step) % count


def send(block, axis, step):
    count = lax.axis_size(axis)
    return lax.ppermute(block, axis, [(i, partner(i, step, count)) for i in range(count)])


def fetch(block, axis, step):
    count = lax.axis_size(axis)
    return lax.ppermute(block, axis, [(partner(i, step, count), i) for i in range(count)])


def plane_columns(out_grad, cols):
    far, near, tp = (lax.axis_size(a) for a in ("far", "near", "tp"))
    rows = out_grad.shape[0]
    shared = far % tp == 0
    piece = far // tp if shared else far
    base = lax.axis_index("tp") * piece if shared else 0
    me = lax.axis_index("far")
    blocks = []
    for n in range(near):
        for k in range(piece):
            start = (partner(me, base + k, far) * near + n) * cols
            blocks.append(lax.dynamic_slice_in_dim(out_grad, start, cols, axis=1))
    blocks = jnp.stack(blocks).reshape(near, piece, rows, cols)
    got = exchange(blocks, "near")
    got = got.transpose(1, 0, 2, 3)
    if shared:
        got = spread_out(got, "tp")
    return got.reshape(far, near * rows, cols)


def on_device(value_in, gate_in, taps, norm_gain, norm_bias, proj_weight, out_grad):
    f32 = jnp.float32
    bf16 = jnp.bfloat16
    rows, local_width = value_in.shape
    span = taps.shape[0]
    half = span // 2
    width_all = local_width * lax.axis_size("tp")
    cols = proj_weight.shape[1]
    far = lax.axis_size("far")
    near = lax.axis_size("near")

    fetched = [fetch(proj_weight, "far", d) for d in reversed(range(1, far))]
    weight_far = jnp.stack([proj_weight] + fetched[::-1])
    grads = plane_columns(out_grad, cols)

    gate_sig = jax.nn.sigmoid(gate_in.astype(f32))
    value_f = value_in.astype(f32)
    mixed = (value_f * gate_sig).astype(bf16)
    padded = padded_2(mixed, SP, half).astype(f32)
    conv = jnp.zeros((rows, local_width), f32)
    for k in range(span):
        conv = conv + taps[k] * padded[k : k + rows]
    mean = lax.psum(jnp.sum(conv, axis=1), "tp") / width_all
    centred = conv - mean[:, None]
    spread = lax.psum(jnp.sum(centred * centred, axis=1), "tp") / width_all
    inv = lax.rsqrt(spread + 1e-06)
    normed = centred * inv[:, None]
    pre = normed * norm_gain + norm_bias
    act = jax.nn.silu(pre).astype(bf16)

    act, grads = lax.optimization_barrier((act, grads))
    act_near = spread_out(act, "near")

    partial = lax.dot_general(
        grads, weight_far, (((0, 2), (0, 2)), ((), ())), preferred_element_type=f32
    ).astype(bf16).reshape(near, rows, local_width)
    grad_parts = exchange(partial, "near")
    act_grad = jnp.sum(grad_parts.astype(f32), axis=0)

    act_near = act_near.reshape(near * rows, local_width)
    weight_grad = None
    for d in reversed(range(far)):
        part = lax.dot_general(
            act_near, grads[d], (((0,), (0,)), ((), ())), preferred_element_type=f32
        )
        part = part.astype(bf16) if d else part
        if d:
            part = send(part, "far", d).astype(f32)
        weight_grad = part if weight_grad is None else weight_grad + part

    sig_pre = jax.nn.sigmoid(pre)
    pre_grad = act_grad * sig_pre * (1.0 + pre * (1.0 - sig_pre))
    normed_grad = pre_grad * norm_gain
    first, second = lax.psum(
        (jnp.sum(normed_grad, axis=1), jnp.sum(normed_grad * normed, axis=1)), "tp"
    )
    conv_grad = inv[:, None] * (
        normed_grad - first[:, None] / width_all - normed * second[:, None] / width_all
    )
    extended = padded_2(conv_grad, SP, half)
    sums = [jnp.sum(conv_grad * padded[k : k + rows], axis=0) for k in range(span)]
    sums.append(jnp.sum(pre_grad * normed, axis=0))
    sums.append(jnp.sum(pre_grad, axis=0))
    totals = sum_over(jnp.stack(sums), SP)
    mixed_grad = jnp.zeros((rows, local_width), f32)
    for k in range(span):
        mixed_grad = mixed_grad + taps[k] * extended[2 * half - k : 2 * half - k + rows]
    value_grad = (mixed_grad * gate_sig).astype(bf16)
    gate_grad = (mixed_grad * value_f * gate_sig * (1.0 - gate_sig)).astype(bf16)
    return (value_grad, gate_grad, totals[:span], totals[span], totals[span + 1], weight_grad)


def solution(mesh):
    count, tp = mesh.shape["sp"], mesh.shape["tp"]
    near = max(d for d in range(1, count + 1) if count % d == 0 and d * d <= count)
    grid = Mesh(mesh.devices.reshape(count // near, near, tp), ("far", "near", "tp"))
    return jax.shard_map(
        on_device,
        mesh=grid,
        in_specs=(
            P(SP, "tp"),
            P(SP, "tp"),
            P(None, "tp"),
            P("tp"),
            P("tp"),
            P("tp", SP),
            P(SP, None),
        ),
        out_specs=(P(SP, "tp"), P(SP, "tp"), P(None, "tp"), P("tp"), P("tp"), P("tp", SP)),
        check_vma=False,
    )
```

```python
import jax
import jax.numpy as jnp
from jax import lax
from jax.experimental import pallas as pl
from jax.experimental.pallas import tpu as pltpu
from jax.sharding import Mesh, PartitionSpec as P


SP = ("far", "near")


def padded_2(cells, axis, width):
    count = lax.axis_size(axis)
    ends = count - 1
    head = lax.slice_in_dim(cells, 0, width, axis=0)
    tail = lax.slice_in_dim(cells, cells.shape[0] - width, cells.shape[0], axis=0)
    return jnp.concatenate(
        [
            lax.ppermute(tail, axis, [(i, (i + 1) % count) for i in range(ends)]),
            cells,
            lax.ppermute(head, axis, [((i + 1) % count, i) for i in range(ends)]),
        ],
        axis=0,
    )


def exchange(blocks, axis):
    return lax.all_to_all(blocks, axis, split_axis=0, concat_axis=0)


def spread_out(block, axis):
    count = lax.axis_size(axis)
    return exchange(jnp.broadcast_to(block[None], (count,) + block.shape), axis)


def sum_over(parts, axis):
    count = lax.axis_size(axis)
    rows, width = parts.shape
    each = -(-rows // count)
    blocks = jnp.pad(parts, ((0, each * count - rows), (0, 0))).reshape(count, each, width)
    blocks = exchange(blocks, axis)
    mine = jnp.sum(blocks, axis=0)
    return spread_out(mine, axis).reshape(each * count, width)[:rows]


def paired(count):
    return count & (count - 1) == 0


def split_of(far, tp):
    shared = far % tp == 0 and paired(far) and paired(tp)
    return (far // tp if shared else far), shared


def partner(row, core, slot, far, tp):
    piece, shared = split_of(far, tp)
    if shared:
        return row ^ slot ^ (core * piece)
    return row ^ slot if paired(far) else (row + slot) % far


def links(slot):
    far, tp = lax.axis_size("far"), lax.axis_size("tp")
    return [
        (row * tp + core, partner(row, core, slot, far, tp) * tp + core)
        for row in range(far)
        for core in range(tp)
    ]


def send(block, slot):
    return lax.ppermute(block, ("far", "tp"), links(slot))


def fetch(block, slot):
    return lax.ppermute(block, ("far", "tp"), [(b, a) for a, b in links(slot)])


def copy_block(places, source, target):
    target[0] = source[...]


def column_blocks(out_grad, places, cols):
    rows = out_grad.shape[0]
    if cols % 128:
        return jnp.stack([lax.dynamic_slice_in_dim(out_grad, p * cols, cols, axis=1) for p in places])
    count = len(places)
    return pl.pallas_call(
        copy_block,
        grid_spec=pltpu.PrefetchScalarGridSpec(
            num_scalar_prefetch=1,
            grid=(count,),
            in_specs=[pl.BlockSpec((rows, cols), lambda g, p: (0, p[g]))],
            out_specs=pl.BlockSpec((1, rows, cols), lambda g, p: (g, 0, 0)),
        ),
        out_shape=jax.ShapeDtypeStruct((count, rows, cols), out_grad.dtype),
        name="column_blocks",
    )(jnp.stack(places), out_grad)


def plane_columns(out_grad, cols):
    far, near, tp = (lax.axis_size(a) for a in ("far", "near", "tp"))
    rows = out_grad.shape[0]
    piece, _ = split_of(far, tp)
    row, core = lax.axis_index("far"), lax.axis_index("tp")
    places = [
        (partner(row, core, k, far, tp) * near + n).astype(jnp.int32)
        for n in range(near)
        for k in range(piece)
    ]
    blocks = column_blocks(out_grad, places, cols).reshape(near, piece, rows, cols)
    got = exchange(blocks, "near")
    return got.transpose(1, 0, 2, 3).reshape(piece, near * rows, cols)


def other_cores(got):
    tp = lax.axis_size("tp")
    if not split_of(lax.axis_size("far"), tp)[1]:
        return got
    swaps = [[(i, i ^ e) for i in range(tp)] for e in range(1, tp)]
    return jnp.concatenate([got] + [lax.ppermute(got, "tp", s) for s in swaps])


def on_device(value_in, gate_in, taps, norm_gain, norm_bias, proj_weight, out_grad):
    f32 = jnp.float32
    bf16 = jnp.bfloat16
    rows, local_width = value_in.shape
    span = taps.shape[0]
    half = span // 2
    width_all = local_width * lax.axis_size("tp")
    cols = proj_weight.shape[1]
    far = lax.axis_size("far")
    near = lax.axis_size("near")

    fetched = [fetch(proj_weight, d) for d in reversed(range(far))]
    weight_far = jnp.stack(fetched[::-1])
    got = plane_columns(out_grad, cols)

    gate_sig = jax.nn.sigmoid(gate_in.astype(f32))
    value_f = value_in.astype(f32)
    mixed = (value_f * gate_sig).astype(bf16)
    padded = padded_2(mixed, SP, half).astype(f32)
    conv = jnp.zeros((rows, local_width), f32)
    for k in range(span):
        conv = conv + taps[k] * padded[k : k + rows]
    mean = lax.psum(jnp.sum(conv, axis=1), "tp") / width_all
    centred = conv - mean[:, None]
    spread = lax.psum(jnp.sum(centred * centred, axis=1), "tp") / width_all
    inv = lax.rsqrt(spread + 1e-06)
    normed = centred * inv[:, None]
    pre = normed * norm_gain + norm_bias
    act = jax.nn.silu(pre).astype(bf16)

    act, got = lax.optimization_barrier((act, got))
    act_near = spread_out(act, "near")
    grads = other_cores(got)

    partial = lax.dot_general(
        grads, weight_far, (((0, 2), (0, 2)), ((), ())), preferred_element_type=f32
    ).astype(bf16).reshape(near, rows, local_width)
    grad_parts = exchange(partial, "near")
    act_grad = jnp.sum(grad_parts.astype(f32), axis=0)

    act_near = act_near.reshape(near * rows, local_width)
    weight_grad = None
    for d in reversed(range(far)):
        part = lax.dot_general(
            act_near, grads[d], (((0,), (0,)), ((), ())), preferred_element_type=f32
        ).astype(bf16)
        part = send(part, d).astype(f32)
        weight_grad = part if weight_grad is None else weight_grad + part

    sig_pre = jax.nn.sigmoid(pre)
    pre_grad = act_grad * sig_pre * (1.0 + pre * (1.0 - sig_pre))
    normed_grad = pre_grad * norm_gain
    first, second = lax.psum(
        (jnp.sum(normed_grad, axis=1), jnp.sum(normed_grad * normed, axis=1)), "tp"
    )
    conv_grad = inv[:, None] * (
        normed_grad - first[:, None] / width_all - normed * second[:, None] / width_all
    )
    extended = padded_2(conv_grad, SP, half)
    sums = [jnp.sum(conv_grad * padded[k : k + rows], axis=0) for k in range(span)]
    sums.append(jnp.sum(pre_grad * normed, axis=0))
    sums.append(jnp.sum(pre_grad, axis=0))
    totals = sum_over(jnp.stack(sums), SP)
    mixed_grad = jnp.zeros((rows, local_width), f32)
    for k in range(span):
        mixed_grad = mixed_grad + taps[k] * extended[2 * half - k : 2 * half - k + rows]
    value_grad = (mixed_grad * gate_sig).astype(bf16)
    gate_grad = (mixed_grad * value_f * gate_sig * (1.0 - gate_sig)).astype(bf16)
    return (value_grad, gate_grad, totals[:span], totals[span], totals[span + 1], weight_grad)


def solution(mesh):
    count, tp = mesh.shape["sp"], mesh.shape["tp"]
    near = max(d for d in range(1, count + 1) if count % d == 0 and d * d <= count)
    grid = Mesh(mesh.devices.reshape(count // near, near, tp), ("far", "near", "tp"))
    return jax.shard_map(
        on_device,
        mesh=grid,
        in_specs=(
            P(SP, "tp"),
            P(SP, "tp"),
            P(None, "tp"),
            P("tp"),
            P("tp"),
            P("tp", SP),
            P(SP, None),
        ),
        out_specs=(P(SP, "tp"), P(SP, "tp"), P(None, "tp"), P("tp"), P("tp"), P("tp", SP)),
        check_vma=False,
    )
```

```python
import jax
import jax.numpy as jnp
from jax import lax
from jax.experimental import pallas as pl
from jax.experimental.pallas import tpu as pltpu
from jax.sharding import Mesh, PartitionSpec as P


SP = ("far", "near")


def padded_2(cells, axis, width):
    count = lax.axis_size(axis)
    ends = count - 1
    head = lax.slice_in_dim(cells, 0, width, axis=0)
    tail = lax.slice_in_dim(cells, cells.shape[0] - width, cells.shape[0], axis=0)
    return jnp.concatenate(
        [
            lax.ppermute(tail, axis, [(i, (i + 1) % count) for i in range(ends)]),
            cells,
            lax.ppermute(head, axis, [((i + 1) % count, i) for i in range(ends)]),
        ],
        axis=0,
    )


def exchange(blocks, axis):
    return lax.all_to_all(blocks, axis, split_axis=0, concat_axis=0)


def spread_out(block, axis):
    count = lax.axis_size(axis)
    return exchange(jnp.broadcast_to(block[None], (count,) + block.shape), axis)


def sum_over(parts, axis):
    count = lax.axis_size(axis)
    rows, width = parts.shape
    each = -(-rows // count)
    blocks = jnp.pad(parts, ((0, each * count - rows), (0, 0))).reshape(count, each, width)
    mine = jnp.sum(exchange(blocks, axis), axis=0)
    return spread_out(mine, axis).reshape(each * count, width)[:rows]


def paired(count):
    return count & (count - 1) == 0


def partner(index, step, count):
    return index ^ step if paired(count) else (index + step) % count


def send(block, axis, step):
    count = lax.axis_size(axis)
    return lax.ppermute(block, axis, [(i, partner(i, step, count)) for i in range(count)])


def fetch(block, axis, step):
    count = lax.axis_size(axis)
    return lax.ppermute(block, axis, [(partner(i, step, count), i) for i in range(count)])


def copy_block(places, source, target):
    target[0] = source[...]


def column_blocks(out_grad, places, cols):
    rows = out_grad.shape[0]
    if cols % 128:
        return jnp.stack([lax.dynamic_slice_in_dim(out_grad, p * cols, cols, axis=1) for p in places])
    count = len(places)
    return pl.pallas_call(
        copy_block,
        grid_spec=pltpu.PrefetchScalarGridSpec(
            num_scalar_prefetch=1,
            grid=(count,),
            in_specs=[pl.BlockSpec((rows, cols), lambda g, p: (0, p[g]))],
            out_specs=pl.BlockSpec((1, rows, cols), lambda g, p: (g, 0, 0)),
        ),
        out_shape=jax.ShapeDtypeStruct((count, rows, cols), out_grad.dtype),
        name="column_blocks",
    )(jnp.stack(places), out_grad)


def plane_columns(out_grad, cols):
    far, near, tp = (lax.axis_size(a) for a in ("far", "near", "tp"))
    rows = out_grad.shape[0]
    shared = far % tp == 0
    piece = far // tp if shared else far
    base = lax.axis_index("tp") * piece if shared else 0
    me = lax.axis_index("far")
    places = [
        jnp.asarray(partner(me, base + k, far) * near + n, jnp.int32)
        for n in range(near)
        for k in range(piece)
    ]
    blocks = column_blocks(out_grad, places, cols).reshape(near, piece, rows, cols)
    got = exchange(blocks, "near")
    got = got.transpose(1, 0, 2, 3)
    if shared:
        got = spread_out(got, "tp")
    return got.reshape(far, near * rows, cols)


def on_device(value_in, gate_in, taps, norm_gain, norm_bias, proj_weight, out_grad):
    f32 = jnp.float32
    bf16 = jnp.bfloat16
    rows, local_width = value_in.shape
    span = taps.shape[0]
    half = span // 2
    width_all = local_width * lax.axis_size("tp")
    cols = proj_weight.shape[1]
    far = lax.axis_size("far")
    near = lax.axis_size("near")

    fetched = [fetch(proj_weight, "far", d) for d in reversed(range(1, far))]
    weight_far = jnp.stack([proj_weight] + fetched[::-1])
    grads = plane_columns(out_grad, cols)

    gate_sig = jax.nn.sigmoid(gate_in.astype(f32))
    value_f = value_in.astype(f32)
    mixed = (value_f * gate_sig).astype(bf16)
    padded = padded_2(mixed, SP, half).astype(f32)
    conv = jnp.zeros((rows, local_width), f32)
    for k in range(span):
        conv = conv + taps[k] * padded[k : k + rows]
    mean = lax.psum(jnp.sum(conv, axis=1), "tp") / width_all
    centred = conv - mean[:, None]
    spread = lax.psum(jnp.sum(centred * centred, axis=1), "tp") / width_all
    inv = lax.rsqrt(spread + 1e-06)
    normed = centred * inv[:, None]
    pre = normed * norm_gain + norm_bias
    act = jax.nn.silu(pre).astype(bf16)

    act, grads = lax.optimization_barrier((act, grads))
    act_near = spread_out(act, "near")

    partial = lax.dot_general(
        grads, weight_far, (((0, 2), (0, 2)), ((), ())), preferred_element_type=f32
    ).astype(bf16).reshape(near, rows, local_width)
    grad_parts = exchange(partial, "near")
    act_grad = jnp.sum(grad_parts.astype(f32), axis=0)

    act_near = act_near.reshape(near * rows, local_width)
    weight_grad = None
    for d in reversed(range(far)):
        part = lax.dot_general(
            act_near, grads[d], (((0,), (0,)), ((), ())), preferred_element_type=f32
        )
        part = part.astype(bf16) if d else part
        if d:
            part = send(part, "far", d).astype(f32)
        weight_grad = part if weight_grad is None else weight_grad + part

    sig_pre = jax.nn.sigmoid(pre)
    pre_grad = act_grad * sig_pre * (1.0 + pre * (1.0 - sig_pre))
    normed_grad = pre_grad * norm_gain
    first, second = lax.psum(
        (jnp.sum(normed_grad, axis=1), jnp.sum(normed_grad * normed, axis=1)), "tp"
    )
    conv_grad = inv[:, None] * (
        normed_grad - first[:, None] / width_all - normed * second[:, None] / width_all
    )
    extended = padded_2(conv_grad, SP, half)
    sums = [jnp.sum(conv_grad * padded[k : k + rows], axis=0) for k in range(span)]
    sums.append(jnp.sum(pre_grad * normed, axis=0))
    sums.append(jnp.sum(pre_grad, axis=0))
    totals = sum_over(jnp.stack(sums), SP)
    mixed_grad = jnp.zeros((rows, local_width), f32)
    for k in range(span):
        mixed_grad = mixed_grad + taps[k] * extended[2 * half - k : 2 * half - k + rows]
    value_grad = (mixed_grad * gate_sig).astype(bf16)
    gate_grad = (mixed_grad * value_f * gate_sig * (1.0 - gate_sig)).astype(bf16)
    return (value_grad, gate_grad, totals[:span], totals[span], totals[span + 1], weight_grad)


def solution(mesh):
    count, tp = mesh.shape["sp"], mesh.shape["tp"]
    near = max(d for d in range(1, count + 1) if count % d == 0 and d * d <= count)
    grid = Mesh(mesh.devices.reshape(count // near, near, tp), ("far", "near", "tp"))
    return jax.shard_map(
        on_device,
        mesh=grid,
        in_specs=(
            P(SP, "tp"),
            P(SP, "tp"),
            P(None, "tp"),
            P("tp"),
            P("tp"),
            P("tp", SP),
            P(SP, None),
        ),
        out_specs=(P(SP, "tp"), P(SP, "tp"), P(None, "tp"), P("tp"), P("tp"), P("tp", SP)),
        check_vma=False,
    )
```
